32 devices in a mesh: sp: 4 (over z), dp: 8 (over y, x, core).
Axes of the slice: x: 2, y: 2, z: 4, core: 2. Of those that a mesh axis runs over, the one named last changes fastest.
Arguments:
- queries: bfloat16 [8, 512, 1024], P('dp', 'sp'), may hold values from -300 to 300
- keys: bfloat16 [8, 512, 1024], P('dp', 'sp'), may hold values from -7 to 7
- values: bfloat16 [8, 512, 1024], P('dp', 'sp'), may hold values from -6 to 6
- cum_gates: float32 [8, 16, 512], P('dp', 'sp'), may hold values from -67 to 0, as said below
- out_weight: bfloat16 [1024, 2048], P(None, 'dp'), may hold values from -0.1875 to 0.1875
Outputs:
- mixed: bfloat16 [8, 512, 2048], P('dp', 'sp')
The draws below stay inside these ranges and needn't reach their ends.
Inputs may be any that keep to these rules, and one draw needn't show every extreme that they name: `cum_gates`: never rises along positions.
All inputs are finite; a program needn't handle non-finite values.
Results may differ from the reference program's by a relative error of at most 0.011.
Values may be sent and summed in bfloat16 or wider, within the bound.
A program may use at most 64 MiB of HBM per device.

```python
import jax
import jax.numpy as jnp
from jax import lax

D = 2048
HEAD_TOTAL = 16
HEAD_DIM = 64
TOK_DEV = 128
SEQUENCE_LENGTH = 512
SEQUENCE_COUNT = 8


def make_pair(key):
    width = HEAD_TOTAL * HEAD_DIM
    queries = jnp.clip(jax.random.normal(jax.random.fold_in(key, 11), (SEQUENCE_COUNT, SEQUENCE_LENGTH, width), jnp.float32), -6.0, 6.0)
    keys = jnp.clip(jax.random.normal(jax.random.fold_in(key, 12), (SEQUENCE_COUNT, SEQUENCE_LENGTH, width), jnp.float32), -6.0, 6.0)
    return (queries, keys)


def draw_queries(key, part):
    return make_pair(key)[0].astype(jnp.bfloat16)


def draw_keys(key, part):
    return make_pair(key)[1].astype(jnp.bfloat16)


def draw_cum_gates(key, part):
    token_position = jnp.arange(SEQUENCE_LENGTH)
    order = jax.random.permutation(jax.random.fold_in(key, 21), HEAD_TOTAL)
    slow_mask = jnp.broadcast_to((order < HEAD_TOTAL // 2)[None, :, None], (SEQUENCE_COUNT, HEAD_TOTAL, 1))
    slow_rate = jax.random.uniform(jax.random.fold_in(key, 22), (SEQUENCE_COUNT, HEAD_TOTAL, 1), jnp.float32, 0.3, 1.0) / SEQUENCE_LENGTH
    fast_rate = jnp.exp(jax.random.uniform(jax.random.fold_in(key, 23), (SEQUENCE_COUNT, HEAD_TOTAL, 1), jnp.float32, jnp.log(1.0 / 100.0), jnp.log(1.0 / 30.0)))
    rate = jnp.where(slow_mask, slow_rate, fast_rate)
    block_count = SEQUENCE_LENGTH // TOK_DEV
    block_factor = jnp.exp(jax.random.uniform(jax.random.fold_in(key, 24), (SEQUENCE_COUNT, 1, block_count), jnp.float32, jnp.log(0.5), jnp.log(2.0)))
    factor = block_factor[:, :, token_position // TOK_DEV]
    rough = jax.random.uniform(jax.random.fold_in(key, 25), (SEQUENCE_COUNT, HEAD_TOTAL, SEQUENCE_LENGTH), jnp.float32, 0.3, 1.7)
    logarithm_gate = -rate * factor * rough
    spike_location = jax.random.randint(jax.random.fold_in(key, 26), (SEQUENCE_COUNT, HEAD_TOTAL, 3), 0, SEQUENCE_LENGTH)
    spike_decrease = jax.random.uniform(jax.random.fold_in(key, 27), (SEQUENCE_COUNT, HEAD_TOTAL, 3), jnp.float32, 0.2, 0.5)
    match_count = (token_position[None, None, None, :] == spike_location[:, :, :, None]).astype(jnp.float32)
    spike_events = jnp.sum(match_count * jnp.log(1.0 - spike_decrease)[:, :, :, None], axis=2)
    return jnp.cumsum(logarithm_gate + spike_events, axis=-1).astype(jnp.float32)


def level_of(rng, extent, pieces, smallest, largest):
    loudness = 1.0
    for position, parts in pieces:
        draws = jax.random.uniform(jax.random.fold_in(jax.random.fold_in(rng, 6), position), (parts,), jnp.float32, smallest / len(pieces), largest / len(pieces))
        loudness = loudness * jnp.repeat(jnp.exp(draws), extent[position] // parts).reshape((-1,) + (1,) * (len(extent) - 1 - position))
    return loudness


def gaussian(rng, dims, spread, limit, split=(), dtype=jnp.bfloat16):
    entries = spread * jax.random.normal(rng, dims, jnp.float32)
    if split:
        entries = entries * level_of(rng, dims, split, -0.22, 0.18)
    return jnp.clip(entries, -limit, limit).astype(dtype)


def setup_inputs(seed: int = 0) -> dict:
    arg_keys = jax.random.split(jax.random.key(seed), 6)
    return {
        "queries": draw_queries(jax.random.fold_in(arg_keys[5], 71), 0),
        "keys": draw_keys(jax.random.fold_in(arg_keys[5], 71), 0),
        "values": gaussian(arg_keys[2], (SEQUENCE_COUNT, SEQUENCE_LENGTH, HEAD_TOTAL * HEAD_DIM), 1.0, 6.0, ((0, 8), (1, 4))),
        "cum_gates": draw_cum_gates(jax.random.fold_in(arg_keys[5], 71), 0),
        "out_weight": gaussian(arg_keys[4], (HEAD_TOTAL * HEAD_DIM, D), (HEAD_TOTAL * HEAD_DIM) ** -0.5, 0.1875, ((1, 8),)),
    }


def attend_sequence(packed, out_weight):
    query_rows, key_rows, value_rows, cum_rows = packed
    length = query_rows.shape[0]
    head_count = cum_rows.shape[0]
    head_size = query_rows.shape[1] // head_count
    query_heads = query_rows.astype(jnp.float32).reshape(length, head_count, head_size).transpose(1, 0, 2)
    key_heads = key_rows.astype(jnp.float32).reshape(length, head_count, head_size).transpose(1, 0, 2)
    value_heads = value_rows.astype(jnp.float32).reshape(length, head_count, head_size).transpose(1, 0, 2)
    scores = jnp.einsum('hqd,hkd->hqk', query_heads, key_heads) * (head_size ** -0.5)
    scores = scores + cum_rows[:, :, None] - cum_rows[:, None, :]
    token_position = jnp.arange(length)
    scores = jnp.where(token_position[None, :] <= token_position[:, None], scores, -jnp.inf)
    row_max = jnp.max(scores, axis=-1, keepdims=True)
    expon = jnp.exp(scores - row_max)
    weights = (expon / jnp.sum(expon, axis=-1, keepdims=True)).astype(jnp.bfloat16)
    head_out = jnp.einsum('hqk,hkd->hqd', weights.astype(jnp.float32), value_heads).astype(jnp.bfloat16)
    head_out = head_out.transpose(1, 0, 2).reshape(length, head_count * head_size)
    return jnp.dot(head_out, out_weight, preferred_element_type=jnp.float32).astype(jnp.bfloat16)


def reference(queries, keys, values, cum_gates, out_weight):
    return lax.map(lambda packed: attend_sequence(packed, out_weight), (queries, keys, values, cum_gates))
```

```python
import functools

import jax
import jax.numpy as jnp
from jax import lax
from jax.experimental import pallas as pl
from jax.experimental.pallas import tpu as pltpu
from jax.sharding import PartitionSpec as P


def attend_heads(query_loc, key_loc, value_loc, cum_loc):
    length = query_loc.shape[0]
    head_count = cum_loc.shape[0]
    head_size = query_loc.shape[1] // head_count
    query_heads = query_loc.reshape(length, head_count, head_size).transpose(1, 0, 2)
    key_heads = key_loc.reshape(length, head_count, head_size).transpose(1, 0, 2)
    value_heads = value_loc.reshape(length, head_count, head_size).transpose(1, 0, 2)
    block_rows = min(512, length)
    block_count = length // block_rows
    query_blocks = query_heads.reshape(head_count, block_count, block_rows, head_size).transpose(
        1, 0, 2, 3
    )
    cum_blocks = cum_loc.reshape(head_count, block_count, block_rows).transpose(1, 0, 2)
    key_pos = jnp.arange(length)
    score_scale = head_size ** (-0.5)

    def one_block(packed):
        query_block, cum_block, block_index = packed
        scores = (
            jnp.einsum("hqd,hkd->hqk", query_block, key_heads, preferred_element_type=jnp.float32)
            * score_scale
        )
        scores = scores + cum_block[:, :, None] - cum_loc[:, None, :]
        query_pos = block_index * block_rows + jnp.arange(block_rows)
        scores = jnp.where(key_pos[None, :] <= query_pos[:, None], scores, -jnp.inf)
        row_max = jnp.max(scores, axis=-1, keepdims=True)
        expon = jnp.exp(scores - row_max)
        weights = (expon / jnp.sum(expon, axis=-1, keepdims=True)).astype(jnp.bfloat16)
        return jnp.einsum(
            "hqk,hkd->hqd", weights, value_heads, preferred_element_type=jnp.float32
        ).astype(jnp.bfloat16)

    results = lax.map(one_block, (query_blocks, cum_blocks, jnp.arange(block_count)))
    return results.transpose(0, 2, 1, 3).reshape(length, head_count * head_size)


def shards(queries, keys, values, cum_gates, out_weight):
    query_loc, key_loc, value_loc = (
        lax.all_to_all(queries[0], "sp", split_axis=1, concat_axis=0, tiled=True),
        lax.all_to_all(keys[0], "sp", split_axis=1, concat_axis=0, tiled=True),
        lax.all_to_all(values[0], "sp", split_axis=1, concat_axis=0, tiled=True),
    )
    head_out = attend_heads(query_loc, key_loc, value_loc, cum_gates[0])
    token_rows = lax.all_to_all(head_out, "sp", split_axis=0, concat_axis=1, tiled=True)
    mixed_rows = jnp.dot(
        token_rows,
        lax.all_gather(out_weight, "dp", axis=1, tiled=True),
        preferred_element_type=jnp.float32,
    )
    return mixed_rows.astype(jnp.bfloat16)[None]


MESH = pl.DeviceIdType.MESH
LANES = 128
HUB = 1
SPLIT = 32


def flip(index, bit):
    return index + bit - 2 * bit * (lax.div(index, bit) % 2)


def attend(c, qs, row_gates, k, v, key_gates, masks, scale, head_size):
    rows = qs[0].shape[0]
    span = k.shape[0]
    lane = lax.broadcasted_iota(jnp.int32, (rows, LANES), 1)
    even = lane < head_size
    picks = [jnp.where(lane % SPLIT == 2 * c + n, 1.0, 0.0).astype(k.dtype) for n in range(2)]
    wide = jnp.concatenate([k, key_gates], axis=1)
    key = lax.broadcasted_iota(jnp.int32, (span, rows), 0) - (span - rows)
    past = key <= lax.broadcasted_iota(jnp.int32, (span, rows), 1)
    scores = []
    for q in qs:
        q = q * jnp.asarray(scale, q.dtype)
        zero = jnp.zeros_like(q)
        stacked = jnp.concatenate(
            [
                jnp.concatenate([jnp.where(even, q, zero), picks[0]], axis=1),
                jnp.concatenate([jnp.where(even, zero, q), picks[1]], axis=1),
            ],
            axis=0,
        )
        scores.append(
            lax.dot_general(
                wide, stacked, (((1,), (1,)), ((), ())), preferred_element_type=jnp.float32
            )
        )
    parts = []
    for score, gate, mask in zip(scores, row_gates, masks):
        for n in range(2):
            part = score[:, n * rows : (n + 1) * rows] + gate[n : n + 1]
            parts.append(jnp.where(past, part, -jnp.inf) if mask else part)
    tops = [jnp.max(part, axis=0, keepdims=True) for part in parts]
    exps = [jnp.exp(part - top) for part, top in zip(parts, tops)]
    totals = [jnp.sum(e, axis=0, keepdims=True) for e in exps]
    results = []
    for i in range(len(qs)):
        probs = jnp.concatenate([exps[2 * i], exps[2 * i + 1]], axis=1).astype(v.dtype)
        sums = lax.dot_general(
            v, probs, (((0,), (0,)), ((), ())), preferred_element_type=jnp.float32
        )
        first = sums[:head_size, :rows] * (1.0 / totals[2 * i])
        second = sums[head_size:, rows:] * (1.0 / totals[2 * i + 1])
        lse = [tops[2 * i + n] + jnp.log(totals[2 * i + n]) for n in range(2)]
        results.append((jnp.concatenate([first, second], axis=0), jnp.concatenate(lse, axis=0)))
    return results


def layer_kernel(
    sizes, q_hbm, k_hbm, v_hbm, g_hbm, w_hbm, out_ref,
    q_own, q_in, kv_own, kv_in, g_in, g_row, g_stage, g_key, o_out, s_out, o_in, s_in, o_own, s_own,
    heads, w_buf, one_part, two_parts,
    in_rs, o_rs, snd, g_rs, g_ss, w_rs, loc, seen_sem,
):
    sp, chunks, head_size, scale = sizes
    z, d = lax.axis_index("sp"), lax.axis_index("dp")
    rows = q_own.shape[0]
    half = w_buf.shape[1] // 2
    core, xs, ys = flip(d, 1), flip(d, 2), flip(d, 4)

    def cols(c):
        return pl.ds(pl.multiple_of(c * LANES, LANES), LANES)

    def remote(src, dst, ss, rs, **device):
        return pltpu.make_async_remote_copy(
            src_ref=src, dst_ref=dst, send_sem=ss, recv_sem=rs,
            device_id=device, device_id_type=MESH,
        )

    def arrived(ref, sem):
        remote(ref, ref, snd.at[0], sem, dp=core).wait_recv()

    def sent(ref, sem):
        remote(ref, ref, sem, w_rs.at[0], dp=core).wait_send()

    local = [
        pltpu.make_async_copy(w_hbm, w_buf.at[0], loc.at[0]),
        pltpu.make_async_copy(q_hbm.at[0], q_own, loc.at[1]),
        pltpu.make_async_copy(k_hbm.at[0], kv_own.at[0], loc.at[2]),
        pltpu.make_async_copy(v_hbm.at[0], kv_own.at[1], loc.at[3]),
        pltpu.make_async_copy(g_hbm.at[0], g_in.at[z], loc.at[4]),
    ]
    for copy in local:
        copy.start()

    barrier = pltpu.get_barrier_semaphore()
    @pl.when(z > 0)
    def _():
        pl.semaphore_signal(barrier, inc=1, device_id={"sp": z - 1}, device_id_type=MESH)

    @pl.when(z < sp - 1)
    def _():
        pl.semaphore_signal(barrier, inc=1, device_id={"sp": z + 1}, device_id_type=MESH)

    for peer in (core, xs, ys):
        pl.semaphore_signal(barrier, inc=1, device_id={"dp": peer}, device_id_type=MESH)
    g_stage[...] = jnp.zeros_like(g_stage)
    pl.semaphore_wait(
        barrier, 3 + (z > 0).astype(jnp.int32) + (z < sp - 1).astype(jnp.int32)
    )

    for teller, pair in ((HUB + 1, (HUB, HUB + 2)), (HUB, (HUB - 1, HUB + 1))):
        @pl.when(z == teller)
        def _():
            for target in pair:
                pl.semaphore_signal(
                    seen_sem.at[teller - HUB], inc=1, device_id={"sp": target},
                    device_id_type=MESH,
                )

    def gate_copy(owner, target, relayed=0):
        return remote(g_in.at[owner], g_in.at[owner], g_ss.at[relayed], g_rs.at[0], sp=target)

    def q_copy(c, slot, target):
        return remote(
            q_own.at[:, cols(c)], q_in.at[slot, :, cols(c)], snd.at[0], in_rs.at[c], sp=target
        )

    def kv_copy(c):
        return remote(
            kv_own.at[:, :, cols(c)], kv_in.at[:, :, cols(c)], snd.at[0], in_rs.at[c], sp=HUB
        )

    whole = {1: 0, 3: 1, 5: 2, 7: 3}
    halves = {2: 4, 4: 6, 6: 8}

    def w_sem(slot, part):
        return w_rs.at[whole[slot] if slot in whole else halves[slot] + part]

    def w_copy(slot, part, bit, peer):
        span = pl.ds(part * half, half)
        return remote(
            w_buf.at[slot, span], w_buf.at[slot ^ bit, span], snd.at[1], w_sem(slot ^ bit, part), dp=peer
        )

    w_plan = {
        "first": [(0, 0, 2, xs), (0, 1, 4, ys), (0, 1, 2, xs), (0, 0, 4, ys), (0, 0, 1, core), (0, 1, 1, core)],
        "early": [(2, 0, 4, ys), (4, 1, 2, xs), (2, 0, 1, core), (4, 1, 1, core)],
        "middle": [(2, 1, 1, core), (4, 0, 1, core)],
        "late": [(6, 0, 1, core), (6, 1, 1, core)],
    }

    def w_arrived(slot, part=None):
        if part is None:
            arrived(w_buf.at[slot], w_sem(slot, 0))
        else:
            arrived(w_buf.at[slot, pl.ds(part * half, half)], w_sem(slot, part))

    def relay(stage):
        seen = []
        for slot, part, bit, peer in w_plan[stage]:
            if slot and (slot, part) not in seen:
                w_arrived(slot, part)
                seen.append((slot, part))
            w_copy(slot, part, bit, peer).start()

    local[0].wait()
    relay("first")
    for copy in local[1:]:
        copy.wait()

    for owner, target in ((0, 1), (1, 0), (1, 2), (2, 1), (2, 3), (3, 2)):
        @pl.when(z == owner)
        def _():
            gate_copy(owner, target).start()

    @pl.when(z == 0)
    def _():
        for c in range(chunks):
            kv_copy(c).start()
            if c == 0:
                pl.semaphore_wait(seen_sem.at[0], 1)
                gate_copy(0, 2).start()

    @pl.when(z == HUB + 1)
    def _():
        for c in range(chunks):
            q_copy(c, 0, HUB).start()
            if c == 0:
                pl.semaphore_wait(seen_sem.at[0], 1)
                gate_copy(2, 0).start()

    @pl.when(z == HUB + 2)
    def _():
        q_copy(0, 1, HUB + 1).start()
        pl.semaphore_wait(seen_sem.at[1], 1)
        gate_copy(3, 1).start()
        q_copy(0, 1, HUB).start()
        q_copy(1, 1, HUB).start()
        for c in range(1, chunks):
            q_copy(c, 1, HUB + 1).start()
            if c + 1 < chunks:
                q_copy(c + 1, 1, HUB).start()

    @pl.when(z == HUB)
    def _():
        pl.semaphore_wait(seen_sem.at[1], 1)
        gate_copy(1, 3).start()

    arrived(g_in.at[pl.ds(0, sp - 1)], g_rs.at[0])

    @pl.when(z == HUB)
    def _():
        gate_copy(0, 3, 1).start()
        gate_copy(3, 0, 1).start()

    per = g_in.shape[1]
    for c in range(chunks):
        for n in range(2):
            head = 2 * c + n
            g_row[c, n : n + 1, :] = g_in[head // per, head % per : head % per + 1, :]

    def key_gates(block):
        for owner in range(sp):
            rest = -g_in[owner, :, pl.ds(pl.multiple_of(block * rows, LANES), rows)]
            for n in range(3):
                piece = rest.astype(jnp.bfloat16).astype(jnp.float32)
                rest = rest - piece
                at = n * SPLIT + owner * per
                g_stage[at : at + per, :] = piece
        return g_stage[...].T.astype(g_key.dtype)

    g_key[1] = key_gates(z)

    @pl.when(z == HUB)
    def _():
        g_key[0] = key_gates(0)

    def work(c, qs, blocks, both, masks):
        k = kv_own[0, :, cols(c)]
        v = kv_own[1, :, cols(c)]
        gates = g_key[1]
        if both:
            k = jnp.concatenate([kv_in[0, :, cols(c)], k], axis=0)
            v = jnp.concatenate([kv_in[1, :, cols(c)], v], axis=0)
            gates = jnp.concatenate([g_key[0], gates], axis=0)
        row_gates = [
            g_row[c, :, pl.ds(pl.multiple_of(block * rows, LANES), rows)] for block in blocks
        ]
        return attend(
            c, [q[:, cols(c)] for q in qs], row_gates, k, v, gates, masks, scale, head_size
        )

    def finish(c, result):
        heads[:, cols(c)] = result.astype(heads.dtype).T

    def put(c, slot, result, lse):
        o_out[slot, c] = result.astype(o_out.dtype)
        s_out[slot, c] = lse

    def give(c, slot, into, target):
        remote(s_out.at[slot, c], s_in.at[into, c], snd.at[3], o_rs.at[c], sp=target).start()
        remote(o_out.at[slot, c], o_in.at[into, c], snd.at[2], o_rs.at[c], sp=target).start()

    @pl.when(z == 0)
    def _():
        @pl.loop(0, chunks // 2)
        def _(pair):
            for n in range(2):
                c = 2 * pair + n
                finish(c, work(c, [q_own], [z], False, [True])[0][0])

        relay("early")
        relay("middle")

    @pl.when(z == HUB)
    def _():
        @pl.loop(0, chunks)
        def _(c):
            @pl.when(c == chunks // 2)
            def _():
                relay("early")

            arrived(w_buf.at[0, pl.ds(0, 2 * rows)], in_rs.at[c])
            far, near, own = work(
                c, [q_in.at[1], q_in.at[0], q_own], [HUB + 2, HUB + 1, HUB], True, [False, False, True]
            )
            put(c, 1, *far)
            put(c, 0, *near)
            give(c, 1, 0, HUB + 2)
            give(c, 0, 0, HUB + 1)
            finish(c, own[0])

        relay("middle")

    @pl.when(z == HUB + 1)
    def _():
        @pl.loop(0, chunks)
        def _(c):
            @pl.when(c == chunks // 2)
            def _():
                relay("early")

            arrived(q_in.at[1, :, cols(c)], in_rs.at[c])
            far, own = work(c, [q_in.at[1], q_own], [HUB + 2, HUB + 1], False, [False, True])
            put(c, 1, *far)
            give(c, 1, 1, HUB + 2)
            o_own[c], s_own[c] = own

    @pl.when(z == HUB + 2)
    def _():
        @pl.loop(0, chunks // 2)
        def _(pair):
            for n in range(2):
                c = 2 * pair + n
                o_own[c], s_own[c] = work(c, [q_own], [z], False, [True])[0]

        relay("early")

    def merge(c, *pieces):
        top = functools.reduce(jnp.maximum, [lse for _, lse in pieces])
        scales = [jnp.exp(lse - top) for _, lse in pieces]
        total = 1.0 / functools.reduce(jnp.add, scales)
        scales = [scale * total for scale in scales]
        blocks = []
        for n in range(2):
            span = slice(n * head_size, (n + 1) * head_size)
            terms = [
                result[span].astype(jnp.float32) * scale[n : n + 1]
                for (result, _), scale in zip(pieces, scales)
            ]
            blocks.append(functools.reduce(jnp.add, terms))
        finish(c, jnp.concatenate(blocks, axis=0))

    @pl.when(z == HUB + 1)
    def _():
        @pl.loop(0, chunks)
        def _(c):
            @pl.when(c == chunks - 2)
            def _():
                relay("middle")

            arrived(one_part, o_rs.at[c])
            merge(c, (o_own[c], s_own[c]), (o_in[0, c], s_in[0, c]))

    @pl.when(z == HUB + 2)
    def _():
        @pl.loop(0, chunks)
        def _(c):
            @pl.when(c == chunks - 2)
            def _():
                relay("middle")

            arrived(two_parts, o_rs.at[c])
            merge(c, (o_own[c], s_own[c]), (o_in[0, c], s_in[0, c]), (o_in[1, c], s_in[1, c]))

    width = w_buf.shape[2]

    def project(slot):
        owner = d
        for bit in (1, 2, 4):
            if slot & bit:
                owner = flip(owner, bit)
        block = jnp.dot(heads[...], w_buf[slot], preferred_element_type=jnp.float32)
        out_ref[0, :, pl.ds(pl.multiple_of(owner * width, LANES), width)] = block.astype(
            out_ref.dtype
        )

    project(0)
    w_arrived(1)
    for slot in (1, 2, 4):
        project(slot)
    for slot in (3, 5):
        w_arrived(slot)
        project(slot)
    relay("late")
    project(6)
    w_arrived(7)
    project(7)

    sent(w_buf.at[pl.ds(0, 7)], snd.at[1])

    @pl.when((z == 0) | (z == HUB + 2))
    def _():
        sent(g_in.at[pl.ds(0, 2)], g_ss.at[0])
        sent(kv_own, snd.at[0])

    @pl.when((z == HUB) | (z == HUB + 1))
    def _():
        sent(g_in.at[pl.ds(0, 3)], g_ss.at[0])

    @pl.when(z == HUB)
    def _():
        sent(g_in.at[pl.ds(0, 2)], g_ss.at[1])
        sent(o_out, snd.at[2])
        sent(s_out, snd.at[3])

    @pl.when(z == HUB + 1)
    def _():
        sent(q_own, snd.at[0])
        sent(o_out.at[1], snd.at[2])
        sent(s_out.at[1], snd.at[3])


def fused_shards(sp, queries, keys, values, cum_gates, out_weight):
    _, rows, width = queries.shape
    _, per, length = cum_gates.shape
    head_size = width // (per * sp)
    depth, block = out_weight.shape
    dp = 8
    chunks = width // LANES
    bf16, f32 = queries.dtype, jnp.float32
    dma = pltpu.SemaphoreType.DMA
    return pl.pallas_call(
        functools.partial(layer_kernel, (sp, chunks, head_size, head_size ** (-0.5))),
        out_shape=jax.ShapeDtypeStruct((1, rows, block * dp), bf16),
        in_specs=[pl.BlockSpec(memory_space=pltpu.HBM)] * 5,
        out_specs=pl.BlockSpec(memory_space=pltpu.VMEM),
        scratch_shapes=[
            pltpu.VMEM((rows, width), bf16),
            pltpu.VMEM((2, rows, width), bf16),
            pltpu.VMEM((2, rows, width), bf16),
            pltpu.VMEM((2, rows, width), bf16),
            pltpu.VMEM((sp, per, length), f32),
            pltpu.VMEM((chunks, 2, length), f32),
            pltpu.VMEM((LANES, rows), f32),
            pltpu.VMEM((2, rows, LANES), bf16),
            pltpu.VMEM((2, chunks, LANES, rows), bf16),
            pltpu.VMEM((2, chunks, 2, rows), f32),
            pltpu.VMEM((2, chunks, LANES, rows), bf16),
            pltpu.VMEM((2, chunks, 2, rows), f32),
            pltpu.VMEM((chunks, LANES, rows), f32),
            pltpu.VMEM((chunks, 2, rows), f32),
            pltpu.VMEM((rows, width), bf16),
            pltpu.VMEM((dp, depth, block), bf16),
            pltpu.VMEM((LANES // 4 + 1, 2, rows), f32),
            pltpu.VMEM((LANES // 2 + 2, 2, rows), f32),
            dma((chunks,)), dma((chunks,)), dma((4,)), dma((1,)), dma((2,)), dma((10,)), dma((5,)),
            pltpu.SemaphoreType.REGULAR((2,)),
        ],
        compiler_params=pltpu.CompilerParams(collective_id=0, has_side_effects=True, vmem_limit_bytes=16 * 2**20),
        name="layer",
    )(*(pltpu.with_memory_space_constraint(x, pltpu.HBM) for x in (queries, keys, values, cum_gates, out_weight)))


def route(sp, dp, queries, keys, values, cum_gates, out_weight):
    _, rows, width = queries.shape
    head_size = width // (cum_gates.shape[1] * sp)
    fits = (
        sp == HUB + 3
        and dp == 8
        and rows == LANES
        and 2 * head_size == LANES
        and width % (2 * LANES) == 0
        and cum_gates.shape[1] * sp <= SPLIT
        and out_weight.shape[1] % (2 * LANES) == 0
    )
    if fits:
        return fused_shards(sp, queries, keys, values, cum_gates, out_weight)
    return shards(queries, keys, values, cum_gates, out_weight)


def solution(mesh):
    in_specs = (
        P("dp", "sp", None),
        P("dp", "sp", None),
        P("dp", "sp", None),
        P("dp", "sp", None),
        P(None, "dp"),
    )
    out_specs = P("dp", "sp", None)
    body = functools.partial(route, mesh.shape["sp"], mesh.shape["dp"])
    return jax.shard_map(body, mesh=mesh, in_specs=in_specs, out_specs=out_specs, check_vma=False)
```

```python
import functools

import jax
import jax.numpy as jnp
from jax import lax
from jax.experimental import pallas as pl
from jax.experimental.pallas import tpu as pltpu
from jax.sharding import PartitionSpec as P


def attend_heads(query_loc, key_loc, value_loc, cum_loc):
    length = query_loc.shape[0]
    head_count = cum_loc.shape[0]
    head_size = query_loc.shape[1] // head_count
    query_heads = query_loc.reshape(length, head_count, head_size).transpose(1, 0, 2)
    key_heads = key_loc.reshape(length, head_count, head_size).transpose(1, 0, 2)
    value_heads = value_loc.reshape(length, head_count, head_size).transpose(1, 0, 2)
    block_rows = min(512, length)
    block_count = length // block_rows
    query_blocks = query_heads.reshape(head_count, block_count, block_rows, head_size).transpose(
        1, 0, 2, 3
    )
    cum_blocks = cum_loc.reshape(head_count, block_count, block_rows).transpose(1, 0, 2)
    key_pos = jnp.arange(length)
    score_scale = head_size ** (-0.5)

    def one_block(packed):
        query_block, cum_block, block_index = packed
        scores = (
            jnp.einsum("hqd,hkd->hqk", query_block, key_heads, preferred_element_type=jnp.float32)
            * score_scale
        )
        scores = scores + cum_block[:, :, None] - cum_loc[:, None, :]
        query_pos = block_index * block_rows + jnp.arange(block_rows)
        scores = jnp.where(key_pos[None, :] <= query_pos[:, None], scores, -jnp.inf)
        row_max = jnp.max(scores, axis=-1, keepdims=True)
        expon = jnp.exp(scores - row_max)
        weights = (expon / jnp.sum(expon, axis=-1, keepdims=True)).astype(jnp.bfloat16)
        return jnp.einsum(
            "hqk,hkd->hqd", weights, value_heads, preferred_element_type=jnp.float32
        ).astype(jnp.bfloat16)

    results = lax.map(one_block, (query_blocks, cum_blocks, jnp.arange(block_count)))
    return results.transpose(0, 2, 1, 3).reshape(length, head_count * head_size)


def shards(queries, keys, values, cum_gates, out_weight):
    query_loc, key_loc, value_loc = (
        lax.all_to_all(queries[0], "sp", split_axis=1, concat_axis=0, tiled=True),
        lax.all_to_all(keys[0], "sp", split_axis=1, concat_axis=0, tiled=True),
        lax.all_to_all(values[0], "sp", split_axis=1, concat_axis=0, tiled=True),
    )
    head_out = attend_heads(query_loc, key_loc, value_loc, cum_gates[0])
    token_rows = lax.all_to_all(head_out, "sp", split_axis=0, concat_axis=1, tiled=True)
    mixed_rows = jnp.dot(
        token_rows,
        lax.all_gather(out_weight, "dp", axis=1, tiled=True),
        preferred_element_type=jnp.float32,
    )
    return mixed_rows.astype(jnp.bfloat16)[None]


MESH = pl.DeviceIdType.MESH
LANES = 128
HUB = 1
SPLIT = 32
EARLY = (0, 1, 2, 4)


def flip(index, bit):
    return index + bit - 2 * bit * (lax.div(index, bit) % 2)


def attend(c, qs, row_gates, k, v, key_gates, masks, scale, head_size):
    rows = qs[0].shape[0]
    span = k.shape[0]
    lane = lax.broadcasted_iota(jnp.int32, (rows, LANES), 1)
    even = lane < head_size
    picks = [jnp.where(lane % SPLIT == 2 * c + n, 1.0, 0.0).astype(k.dtype) for n in range(2)]
    wide = jnp.concatenate([k, key_gates], axis=1)
    key = lax.broadcasted_iota(jnp.int32, (span, rows), 0) - (span - rows)
    past = key <= lax.broadcasted_iota(jnp.int32, (span, rows), 1)
    scores = []
    for q in qs:
        q = q * jnp.asarray(scale, q.dtype)
        zero = jnp.zeros_like(q)
        stacked = jnp.concatenate(
            [
                jnp.concatenate([jnp.where(even, q, zero), picks[0]], axis=1),
                jnp.concatenate([jnp.where(even, zero, q), picks[1]], axis=1),
            ],
            axis=0,
        )
        scores.append(
            lax.dot_general(
                wide, stacked, (((1,), (1,)), ((), ())), preferred_element_type=jnp.float32
            )
        )
    parts = []
    for score, gate, mask in zip(scores, row_gates, masks):
        for n in range(2):
            part = score[:, n * rows : (n + 1) * rows] + gate[n : n + 1]
            parts.append(jnp.where(past, part, -jnp.inf) if mask else part)
    tops = [jnp.max(part, axis=0, keepdims=True) for part in parts]
    exps = [jnp.exp(part - top) for part, top in zip(parts, tops)]
    totals = [jnp.sum(e, axis=0, keepdims=True) for e in exps]
    results = []
    for i in range(len(qs)):
        probs = jnp.concatenate([exps[2 * i], exps[2 * i + 1]], axis=1).astype(v.dtype)
        sums = lax.dot_general(
            v, probs, (((0,), (0,)), ((), ())), preferred_element_type=jnp.float32
        )
        first = sums[:head_size, :rows] * (1.0 / totals[2 * i])
        second = sums[head_size:, rows:] * (1.0 / totals[2 * i + 1])
        lse = [tops[2 * i + n] + jnp.log(totals[2 * i + n]) for n in range(2)]
        results.append((jnp.concatenate([first, second], axis=0), jnp.concatenate(lse, axis=0)))
    return results


def layer_kernel(
    sizes, q_hbm, k_hbm, v_hbm, g_hbm, w_hbm, out_ref,
    q_own, q_in, kv_own, kv_in, g_in, g_row, g_stage, g_key, o_out, s_out, o_in, s_in, o_own, s_own,
    o_far, s_far, total, heads, w_buf, one_part, two_parts,
    in_rs, o_rs, snd, g_rs, g_ss, w_rs, loc, seen_sem,
):
    sp, chunks, head_size, scale = sizes
    z, d = lax.axis_index("sp"), lax.axis_index("dp")
    rows = q_own.shape[0]
    half = w_buf.shape[1] // 2
    core, xs, ys = flip(d, 1), flip(d, 2), flip(d, 4)

    def cols(c):
        return pl.ds(pl.multiple_of(c * LANES, LANES), LANES)

    def remote(src, dst, ss, rs, **device):
        return pltpu.make_async_remote_copy(
            src_ref=src, dst_ref=dst, send_sem=ss, recv_sem=rs,
            device_id=device, device_id_type=MESH,
        )

    def arrived(ref, sem):
        remote(ref, ref, snd.at[0], sem, dp=core).wait_recv()

    def sent(ref, sem):
        remote(ref, ref, sem, w_rs.at[0], dp=core).wait_send()

    local = [
        pltpu.make_async_copy(w_hbm, w_buf.at[0], loc.at[0]),
        pltpu.make_async_copy(q_hbm.at[0], q_own, loc.at[1]),
        pltpu.make_async_copy(k_hbm.at[0], kv_own.at[0], loc.at[2]),
        pltpu.make_async_copy(v_hbm.at[0], kv_own.at[1], loc.at[3]),
        pltpu.make_async_copy(g_hbm.at[0], g_in.at[z], loc.at[4]),
    ]
    for copy in local:
        copy.start()

    barrier = pltpu.get_barrier_semaphore()
    @pl.when(z > 0)
    def _():
        pl.semaphore_signal(barrier, inc=1, device_id={"sp": z - 1}, device_id_type=MESH)

    @pl.when(z < sp - 1)
    def _():
        pl.semaphore_signal(barrier, inc=1, device_id={"sp": z + 1}, device_id_type=MESH)

    for peer in (core, xs, ys):
        pl.semaphore_signal(barrier, inc=1, device_id={"dp": peer}, device_id_type=MESH)
    g_stage[...] = jnp.zeros_like(g_stage)
    pl.semaphore_wait(
        barrier, 3 + (z > 0).astype(jnp.int32) + (z < sp - 1).astype(jnp.int32)
    )

    for teller, pair in ((HUB + 1, (HUB, HUB + 2)), (HUB, (HUB - 1, HUB + 1))):
        @pl.when(z == teller)
        def _():
            for target in pair:
                pl.semaphore_signal(
                    seen_sem.at[teller - HUB], inc=1, device_id={"sp": target},
                    device_id_type=MESH,
                )

    def gate_copy(owner, target, relayed=0):
        late = owner == HUB + 2 and target == HUB
        return remote(
            g_in.at[owner], g_in.at[owner], g_ss.at[relayed], g_rs.at[1 if late else 0], sp=target
        )

    def q_copy(c, slot, target):
        lone = slot == 1 and target == HUB and c == 0
        return remote(
            q_own.at[:, cols(c)], q_in.at[slot, :, cols(c)], snd.at[0],
            in_rs.at[chunks if lone else c], sp=target,
        )

    def kv_copy(c):
        return remote(
            kv_own.at[:, :, cols(c)], kv_in.at[:, :, cols(c)], snd.at[0], in_rs.at[c], sp=HUB
        )

    depth = w_buf.shape[1]
    shed = depth // 8
    odd = z % 2
    parts = {}
    for slot, front, back in ((2, 0, half), (4, half, 0)):
        parts[slot, "first"] = (front, half // 2)
        parts[slot, "second"] = (front + half // 2, half // 2)
        parts[slot, "lent"] = (back + 2 * shed * (1 - odd), 2 * shed)
        parts[slot, "rest"] = (back + shed * (1 + odd), shed)
        parts[slot, "given"] = (back + 3 * shed * odd, shed)
        parts[slot, "swap"] = (back + 3 * shed * (1 - odd), shed)
        parts[slot, "wide"] = (back, 2 * shed)
        parts[slot, "some"] = (back + 5 * shed // 2, 3 * shed // 2)
        parts[slot, "bit"] = (back + 2 * shed, shed // 2)
    alias = {"wide": "given", "some": "given", "bit": "rest"}
    names = ["first", "second", "rest", "lent", "given"]

    for slot in (2, 4):
        start, size = parts[slot, "second"]
        parts[slot, "kept"] = (start, size // 2)
        parts[slot, "moved"] = (start + size // 2, size // 2)
    lasts = ["first", "kept", "moved"]

    def w_sem(slot, name):
        if name is None:
            return w_rs.at[slot // 2]
        if slot in (2, 4):
            return w_rs.at[4 + 5 * (slot == 4) + names.index(name)]
        base = {6: 14, 7: 20, 3: 22, 5: 23}[slot]
        if slot == 6:
            base += lasts.index(name[0]) + 3 * (name[1] == 4)
        if slot == 7:
            base += name[1] == 4
        return w_rs.at[base]

    def w_ref(slot, rows_of):
        start, size = rows_of
        return w_buf.at[slot, pl.ds(pl.multiple_of(start, 16), size)]

    def w_copy(slot, into, rows_of, ss, rs, **device):
        remote(w_ref(slot, rows_of), w_ref(into, rows_of), snd.at[ss], rs, **device).start()

    def w_first():
        def spread(name):
            w_copy(0, 2, parts[2, name], 4, w_sem(2, alias.get(name, name)), dp=xs)
            w_copy(0, 4, parts[4, name], 4, w_sem(4, alias.get(name, name)), dp=ys)

        spread("lent")
        w_copy(0, 1, (0, depth), 1, w_sem(1, None), dp=core)
        spread("first")
        spread("second")

        @pl.when(z > HUB)
        def _():
            spread("rest")

        @pl.when(z == HUB)
        def _():
            spread("bit")

    turns = {2: (4, ys), 4: (2, xs)}

    def w_got(name):
        for slot in (2, 4):
            piece = parts[slot, name]
            arrived(w_ref(slot, piece), w_sem(slot, alias.get(name, name)))
            peer = turns[slot][1]
            if name == "first":
                w_copy(slot, 6, piece, 4, w_sem(6, ("first", slot)), dp=peer)
            if name == "second":
                w_copy(slot, 6, parts[slot, "kept"], 4, w_sem(6, ("kept", slot)), dp=peer)

                @pl.when(d % 2 == 1)
                def _():
                    w_copy(slot, 6, parts[slot, "moved"], 4, w_sem(6, ("moved", slot)), dp=peer)

            into = w_sem(slot + 1, "second" if name == "second" else None)
            w_copy(slot, slot + 1, piece, 1, into, dp=core)

    def w_cross():
        @pl.when(d % 2 == 1)
        def _():
            for slot in (2, 4):
                arrived(w_ref(slot + 1, parts[slot, "second"]), w_sem(slot + 1, "second"))
                w_copy(slot + 1, 7, parts[slot, "moved"], 4, w_sem(7, ("moved", slot)), dp=turns[slot][1])

    def w_lend():
        for giver, sends in (
            (0, [(2, "some", 1)]),
            (1, [(2, "lent", 0), (4, "lent", 0)]),
            (2, [(2, "swap", 3), (4, "swap", 3), (4, "some", 1)]),
            (3, [(2, "swap", 2), (4, "swap", 2)]),
        ):
            @pl.when(z == giver)
            def _():
                for slot, name, target in sends:
                    w_copy(slot, slot, parts[slot, name], 5, w_sem(slot, "given"), sp=target)

    def w_diag(name):
        for slot in (2, 4):
            for part in ("first",) if name == "first" else ("kept",):
                arrived(w_ref(6, parts[slot, part]), w_sem(6, (part, slot)))
                w_copy(6, 7, parts[slot, part], 1, w_sem(7, None), dp=core)
        if name == "second":
            @pl.when(d % 2 == 1)
            def _():
                for slot in (2, 4):
                    piece = parts[slot, "moved"]
                    arrived(w_ref(6, piece), w_sem(6, ("moved", slot)))
                    w_copy(6, 7, piece, 1, w_sem(7, None), dp=core)
                for slot in (2, 4):
                    piece = parts[slot, "moved"]
                    arrived(w_ref(7, piece), w_sem(7, ("moved", slot)))
                    w_copy(7, 6, piece, 1, w_sem(6, ("moved", slot)), dp=core)

    def w_arrived(slot):
        if slot == 1:
            arrived(w_buf.at[slot], w_sem(slot, None))
            return
        short = w_buf.at[slot, pl.ds(0, depth - 2 * shed)]
        if slot == 7:
            @pl.when(d % 2 == 0)
            def _():
                arrived(w_buf.at[slot], w_sem(slot, None))
                for near in (2, 4):
                    arrived(w_ref(6, parts[near, "moved"]), w_sem(6, ("moved", near)))

            @pl.when(d % 2 == 1)
            def _():
                arrived(short, w_sem(slot, None))
            return
        arrived(short, w_sem(slot, None))

        @pl.when(d % 2 == 0)
        def _():
            arrived(w_ref(slot, parts[slot - 1, "second"]), w_sem(slot, "second"))

    local[0].wait()
    w_first()
    for copy in local[1:]:
        copy.wait()

    for owner, target in ((0, 1), (1, 0), (1, 2), (2, 1), (2, 3), (3, 2)):
        @pl.when(z == owner)
        def _():
            gate_copy(owner, target).start()

    @pl.when(z == 0)
    def _():
        for c in range(chunks):
            kv_copy(c).start()
            if c == 0:
                pl.semaphore_wait(seen_sem.at[0], 1)
                gate_copy(0, 2).start()

    @pl.when(z == HUB + 1)
    def _():
        for c in range(chunks):
            q_copy(c, 0, HUB).start()
            if c == 0:
                pl.semaphore_wait(seen_sem.at[0], 1)
                gate_copy(2, 0).start()

    @pl.when(z == HUB + 2)
    def _():
        q_copy(0, 1, HUB + 1).start()
        pl.semaphore_wait(seen_sem.at[1], 1)
        gate_copy(3, 1).start()
        q_copy(0, 1, HUB).start()
        q_copy(1, 1, HUB).start()
        for c in range(1, chunks):
            q_copy(c, 1, HUB + 1).start()
            if c + 1 < chunks:
                q_copy(c + 1, 1, HUB).start()

    @pl.when(z == HUB)
    def _():
        pl.semaphore_wait(seen_sem.at[1], 1)
        gate_copy(1, 3).start()

    @pl.when(z != HUB)
    def _():
        w_got("lent")
        w_lend()

    @pl.when(z == 0)
    def _():
        w_got("first")

    @pl.when(z == HUB)
    def _():
        arrived(g_in.at[pl.ds(0, sp - 2)], g_rs.at[0])

    @pl.when(z != HUB)
    def _():
        arrived(g_in.at[pl.ds(0, sp - 1)], g_rs.at[0])

    per = g_in.shape[1]

    def row_gates(owners):
        for owner in owners:
            for at in range(per):
                c, n = divmod(owner * per + at, 2)
                g_row[c, n : n + 1, :] = g_in[owner, at : at + 1, :]

    def key_gates(block, owners):
        for owner in owners:
            rest = -g_in[owner, :, pl.ds(pl.multiple_of(block * rows, LANES), rows)]
            for n in range(3):
                piece = rest.astype(jnp.bfloat16).astype(jnp.float32)
                rest = rest - piece
                at = n * SPLIT + owner * per
                g_stage[at : at + per, :] = piece
        return g_stage[...].T.astype(g_key.dtype)

    def hub_gates(owners):
        row_gates(owners)
        for n in range(2):
            g_key[n] = key_gates(n + HUB - 1, range(owners[-1] + 1))

    @pl.when(z == HUB)
    def _():
        hub_gates(range(HUB + 2))

    @pl.when(z != HUB)
    def _():
        row_gates(range(sp))
        g_key[1] = key_gates(z, range(sp))

    def work(c, qs, blocks, both, masks):
        k = kv_own[0, :, cols(c)]
        v = kv_own[1, :, cols(c)]
        gates = g_key[1]
        if both:
            k = jnp.concatenate([kv_in[0, :, cols(c)], k], axis=0)
            v = jnp.concatenate([kv_in[1, :, cols(c)], v], axis=0)
            gates = jnp.concatenate([g_key[0], gates], axis=0)
        rows_of = [
            g_row[c, :, pl.ds(pl.multiple_of(block * rows, LANES), rows)] for block in blocks
        ]
        return attend(
            c, [q[:, cols(c)] for q in qs], rows_of, k, v, gates, masks, scale, head_size
        )

    def finish(c, result):
        heads[:, cols(c)] = result.astype(heads.dtype).T

    def put(c, slot, result, lse):
        o_out[slot, c] = result.astype(o_out.dtype)
        s_out[slot, c] = lse

    def give(c, slot, into, target):
        remote(s_out.at[slot, c], s_in.at[into, c], snd.at[3], o_rs.at[c], sp=target).start()
        remote(o_out.at[slot, c], o_in.at[into, c], snd.at[2], o_rs.at[c], sp=target).start()

    def merge(*pieces):
        top = functools.reduce(jnp.maximum, [lse for _, lse in pieces])
        scales = [jnp.exp(lse - top) for _, lse in pieces]
        total = 1.0 / functools.reduce(jnp.add, scales)
        scales = [scale * total for scale in scales]
        blocks = []
        for n in range(2):
            span = slice(n * head_size, (n + 1) * head_size)
            terms = [
                result[span].astype(jnp.float32) * scale[n : n + 1]
                for (result, _), scale in zip(pieces, scales)
            ]
            blocks.append(functools.reduce(jnp.add, terms))
        return jnp.concatenate(blocks, axis=0), top - jnp.log(total)

    def on(c, step, run, *args):
        @pl.when(c == step)
        def _():
            run(*args)

    cut = chunks // 2
    width = w_buf.shape[2]

    def product(slot, start, stop):
        span = pl.ds(start * LANES, (stop - start) * LANES)
        return jnp.dot(heads[:, span], w_buf[slot, span], preferred_element_type=jnp.float32)

    def store(slot, block):
        owner = d
        for bit in (1, 2, 4):
            if slot & bit:
                owner = flip(owner, bit)
        out_ref[0, :, pl.ds(pl.multiple_of(owner * width, LANES), width)] = block.astype(
            out_ref.dtype
        )

    def project(slot):
        store(slot, product(slot, 0, chunks))

    def remain(start):
        for n, slot in enumerate(EARLY):
            store(slot, total[n] + product(slot, start, chunks))

    def gather(stop):
        w_arrived(1)
        for n, slot in enumerate(EARLY):
            if stop == chunks:
                project(slot)
            else:
                total[n] = product(slot, 0, stop)

    def ends(stop):
        @pl.when(d % 2 == 0)
        def _():
            w_diag("second")

        gather(stop)

        @pl.when(d % 2 == 1)
        def _():
            w_diag("second")

    @pl.when(z == 0)
    def _():
        @pl.loop(0, chunks // 2)
        def _(pair):
            for n in range(2):
                c = 2 * pair + n
                finish(c, work(c, [q_own], [z], False, [True])[0][0])

        w_got("second")
        w_got("wide")
        w_cross()
        gather(chunks)
        w_diag("first")
        w_diag("second")

    @pl.when(z == HUB)
    def _():
        def hub(c, joined):
            arrived(w_buf.at[0, pl.ds(0, 2 * rows)], in_rs.at[c])
            far, near, own = work(
                c, [q_in.at[1], q_in.at[0], q_own], [HUB + 2, HUB + 1, HUB], True, [False, False, True]
            )
            put(c, 1, *far)
            put(c, 0, *near)
            if joined:
                give(c, 1, 1, HUB + 1)
            else:
                give(c, 1, 0, HUB + 2)
            give(c, 0, 0, HUB + 1)
            finish(c, own[0])

        arrived(w_buf.at[0, pl.ds(0, 3 * rows // 2)], in_rs.at[0])
        near, own = work(0, [q_in.at[0], q_own], [HUB + 1, HUB], True, [False, True])
        put(0, 0, *near)
        give(0, 0, 0, HUB + 1)
        finish(0, own[0])
        arrived(g_in.at[0], g_rs.at[1])
        gate_copy(0, 3, 1).start()
        gate_copy(3, 0, 1).start()
        hub_gates(range(HUB + 2, sp))
        arrived(w_buf.at[0, pl.ds(0, rows // 2)], in_rs.at[chunks])
        put(0, 1, *work(0, [q_in.at[1]], [HUB + 2], True, [False])[0])
        give(0, 1, 0, HUB + 2)
        w_got("lent")
        w_lend()

        @pl.loop(1, cut + 1)
        def _(c):
            on(c, 3, w_got, "first")
            hub(c, True)

        w_got("second")

        @pl.loop(cut + 1, chunks)
        def _(c):
            @pl.when(c == chunks - 1)
            def _():
                w_got("bit")
                w_cross()
                w_diag("first")

            hub(c, False)

        w_got("some")
        ends(chunks)

    @pl.when(z == HUB + 1)
    def _():
        def near(c, joined):
            arrived(q_in.at[1, :, cols(c)], in_rs.at[c])
            far, own = work(c, [q_in.at[1], q_own], [HUB + 2, HUB + 1], False, [False, True])
            if joined:
                o_far[c - 1], s_far[c - 1] = far
            else:
                put(c, 1, *far)
                give(c, 1, 1, HUB + 2)
            o_own[c], s_own[c] = own

        def join(c, joined):
            arrived(two_parts if joined else one_part, o_rs.at[c])
            if joined:
                put(c, 1, *merge((o_far[c - 1], s_far[c - 1]), (o_in[1, c], s_in[1, c])))
                give(c, 1, 1, HUB + 2)
            finish(c, merge((o_own[c], s_own[c]), (o_in[0, c], s_in[0, c]))[0])

        near(0, False)

        @pl.loop(1, cut + 1)
        def _(c):
            on(c, 3, w_got, "first")
            near(c, True)

        join(0, False)
        join(1, True)

        @pl.loop(cut + 1, chunks)
        def _(c):
            on(c, cut + 1, w_got, "second")

            @pl.when(c == chunks - 1)
            def _():
                w_got("rest")
                w_cross()

            near(c, False)
            join(c - cut + 1, True)

        w_diag("first")
        w_got("given")

        @pl.loop(cut + 1, chunks - 1)
        def _(c):
            join(c, False)

        ends(chunks - 1)
        join(chunks - 1, False)
        remain(chunks - 1)

    @pl.when(z == HUB + 2)
    def _():
        @pl.loop(0, chunks // 2)
        def _(pair):
            for n in range(2):
                c = 2 * pair + n
                o_own[c], s_own[c] = work(c, [q_own], [z], False, [True])[0]

        def join(c, joined):
            arrived(one_part if joined else two_parts, o_rs.at[c])
            pieces = [(o_own[c], s_own[c]), (o_in[1, c], s_in[1, c])]
            if not joined:
                pieces.append((o_in[0, c], s_in[0, c]))
            finish(c, merge(*pieces)[0])

        w_got("first")
        w_got("second")
        w_got("rest")
        w_cross()
        w_diag("first")
        w_got("given")
        join(0, False)

        @pl.loop(1, cut - 1)
        def _(c):
            join(c, True)

        @pl.when(d % 2 == 0)
        def _():
            w_diag("second")

        join(cut - 1, True)
        gather(cut)

        @pl.when(d % 2 == 1)
        def _():
            w_diag("second")

        join(cut, True)

        @pl.loop(cut + 1, chunks)
        def _(c):
            join(c, False)

        w_arrived(3)
        w_arrived(5)
        w_arrived(7)
        remain(cut)
        for slot in (3, 5, 6, 7):
            project(slot)

    @pl.when(z <= HUB + 1)
    def _():
        for slot in (3, 5):
            w_arrived(slot)
        for slot in (3, 5):
            project(slot)
        w_arrived(7)
        for slot in (6, 7):
            project(slot)

    for parity in range(2):
        @pl.when(d % 2 == parity)
        def _():
            moved = (2 * parity - 1) * shed
            sent(w_buf.at[:, pl.ds(0, depth // 2 + moved // 4)], snd.at[1])
            for plane in range(sp):
                @pl.when(z == plane)
                def _():
                    each = 5 * depth // 8 + (0, shed // 4, shed // 2, shed // 2)[plane] + moved // 2
                    sent(w_buf.at[pl.ds(0, 4), pl.ds(0, each)], snd.at[4])

    for giver, count in enumerate((3, 8, 7, 4)):
        @pl.when(z == giver)
        def _():
            sent(w_buf.at[0, pl.ds(0, count * shed // 2)], snd.at[5])

    @pl.when((z == 0) | (z == HUB + 2))
    def _():
        sent(g_in.at[pl.ds(0, 2)], g_ss.at[0])
        sent(kv_own, snd.at[0])

    @pl.when((z == HUB) | (z == HUB + 1))
    def _():
        sent(g_in.at[pl.ds(0, 3)], g_ss.at[0])

    @pl.when(z == HUB)
    def _():
        sent(g_in.at[pl.ds(0, 2)], g_ss.at[1])
        sent(o_out, snd.at[2])
        sent(s_out, snd.at[3])

    @pl.when(z == HUB + 1)
    def _():
        sent(q_own, snd.at[0])
        sent(o_out.at[1], snd.at[2])
        sent(s_out.at[1], snd.at[3])


def fused_shards(sp, queries, keys, values, cum_gates, out_weight):
    _, rows, width = queries.shape
    _, per, length = cum_gates.shape
    head_size = width // (per * sp)
    depth, block = out_weight.shape
    dp = 8
    chunks = width // LANES
    bf16, f32 = queries.dtype, jnp.float32
    dma = pltpu.SemaphoreType.DMA
    return pl.pallas_call(
        functools.partial(layer_kernel, (sp, chunks, head_size, head_size ** (-0.5))),
        out_shape=jax.ShapeDtypeStruct((1, rows, block * dp), bf16),
        in_specs=[pl.BlockSpec(memory_space=pltpu.HBM)] * 5,
        out_specs=pl.BlockSpec(memory_space=pltpu.VMEM),
        scratch_shapes=[
            pltpu.VMEM((rows, width), bf16),
            pltpu.VMEM((2, rows, width), bf16),
            pltpu.VMEM((2, rows, width), bf16),
            pltpu.VMEM((2, rows, width), bf16),
            pltpu.VMEM((sp, per, length), f32),
            pltpu.VMEM((chunks, 2, length), f32),
            pltpu.VMEM((LANES, rows), f32),
            pltpu.VMEM((2, rows, LANES), bf16),
            pltpu.VMEM((2, chunks, LANES, rows), bf16),
            pltpu.VMEM((2, chunks, 2, rows), f32),
            pltpu.VMEM((2, chunks, LANES, rows), bf16),
            pltpu.VMEM((2, chunks, 2, rows), f32),
            pltpu.VMEM((chunks, LANES, rows), f32),
            pltpu.VMEM((chunks, 2, rows), f32),
            pltpu.VMEM((chunks // 2, LANES, rows), f32),
            pltpu.VMEM((chunks // 2, 2, rows), f32),
            pltpu.VMEM((len(EARLY), rows, block), f32),
            pltpu.VMEM((rows, width), bf16),
            pltpu.VMEM((dp, depth, block), bf16),
            pltpu.VMEM((LANES // 4 + 1, 2, rows), f32),
            pltpu.VMEM((LANES // 2 + 2, 2, rows), f32),
            dma((chunks + 1,)), dma((chunks,)), dma((6,)), dma((2,)), dma((2,)), dma((24,)), dma((5,)),
            pltpu.SemaphoreType.REGULAR((2,)),
        ],
        compiler_params=pltpu.CompilerParams(collective_id=0, has_side_effects=True, vmem_limit_bytes=16 * 2**20),
        name="layer",
    )(*(pltpu.with_memory_space_constraint(x, pltpu.HBM) for x in (queries, keys, values, cum_gates, out_weight)))


def route(sp, dp, queries, keys, values, cum_gates, out_weight):
    _, rows, width = queries.shape
    head_size = width // (cum_gates.shape[1] * sp)
    fits = (
        sp == HUB + 3
        and dp == 8
        and rows == LANES
        and 2 * head_size == LANES
        and width == 8 * LANES
        and out_weight.shape[0] % (2 * LANES) == 0
        and cum_gates.shape[1] * sp <= SPLIT
        and out_weight.shape[1] % (2 * LANES) == 0
    )
    if fits:
        return fused_shards(sp, queries, keys, values, cum_gates, out_weight)
    return shards(queries, keys, values, cum_gates, out_weight)


def solution(mesh):
    in_specs = (
        P("dp", "sp", None),
        P("dp", "sp", None),
        P("dp", "sp", None),
        P("dp", "sp", None),
        P(None, "dp"),
    )
    out_specs = P("dp", "sp", None)
    body = functools.partial(route, mesh.shape["sp"], mesh.shape["dp"])
    return jax.shard_map(body, mesh=mesh, in_specs=in_specs, out_specs=out_specs, check_vma=False)
```

```python
import functools

import jax
import jax.numpy as jnp
from jax import lax
from jax.experimental import pallas as pl
from jax.experimental.pallas import tpu as pltpu
from jax.sharding import PartitionSpec as P


def attend_heads(query_loc, key_loc, value_loc, cum_loc):
    length = query_loc.shape[0]
    head_count = cum_loc.shape[0]
    head_size = query_loc.shape[1] // head_count
    query_heads = query_loc.reshape(length, head_count, head_size).transpose(1, 0, 2)
    key_heads = key_loc.reshape(length, head_count, head_size).transpose(1, 0, 2)
    value_heads = value_loc.reshape(length, head_count, head_size).transpose(1, 0, 2)
    block_rows = min(512, length)
    block_count = length // block_rows
    query_blocks = query_heads.reshape(head_count, block_count, block_rows, head_size).transpose(
        1, 0, 2, 3
    )
    cum_blocks = cum_loc.reshape(head_count, block_count, block_rows).transpose(1, 0, 2)
    key_pos = jnp.arange(length)
    score_scale = head_size ** (-0.5)

    def one_block(packed):
        query_block, cum_block, block_index = packed
        scores = (
            jnp.einsum("hqd,hkd->hqk", query_block, key_heads, preferred_element_type=jnp.float32)
            * score_scale
        )
        scores = scores + cum_block[:, :, None] - cum_loc[:, None, :]
        query_pos = block_index * block_rows + jnp.arange(block_rows)
        scores = jnp.where(key_pos[None, :] <= query_pos[:, None], scores, -jnp.inf)
        row_max = jnp.max(scores, axis=-1, keepdims=True)
        expon = jnp.exp(scores - row_max)
        weights = (expon / jnp.sum(expon, axis=-1, keepdims=True)).astype(jnp.bfloat16)
        return jnp.einsum(
            "hqk,hkd->hqd", weights, value_heads, preferred_element_type=jnp.float32
        ).astype(jnp.bfloat16)

    results = lax.map(one_block, (query_blocks, cum_blocks, jnp.arange(block_count)))
    return results.transpose(0, 2, 1, 3).reshape(length, head_count * head_size)


def shards(queries, keys, values, cum_gates, out_weight):
    query_loc, key_loc, value_loc = (
        lax.all_to_all(queries[0], "sp", split_axis=1, concat_axis=0, tiled=True),
        lax.all_to_all(keys[0], "sp", split_axis=1, concat_axis=0, tiled=True),
        lax.all_to_all(values[0], "sp", split_axis=1, concat_axis=0, tiled=True),
    )
    head_out = attend_heads(query_loc, key_loc, value_loc, cum_gates[0])
    token_rows = lax.all_to_all(head_out, "sp", split_axis=0, concat_axis=1, tiled=True)
    mixed_rows = jnp.dot(
        token_rows,
        lax.all_gather(out_weight, "dp", axis=1, tiled=True),
        preferred_element_type=jnp.float32,
    )
    return mixed_rows.astype(jnp.bfloat16)[None]


MESH = pl.DeviceIdType.MESH
LANES = 128
HUB = 1
SPLIT = 32
EARLY = (0, 1, 2, 4)
JOINED = (2, 5)
THIN = 4


def flip(index, bit):
    return index + bit - 2 * bit * (lax.div(index, bit) % 2)


def attend(c, qs, row_gates, k, v, key_gates, masks, scale, head_size):
    rows = qs[0].shape[0]
    span = k.shape[0]
    lane = lax.broadcasted_iota(jnp.int32, (rows, LANES), 1)
    even = lane < head_size
    picks = [jnp.where(lane % SPLIT == 2 * c + n, 1.0, 0.0).astype(k.dtype) for n in range(2)]
    wide = jnp.concatenate([k, key_gates], axis=1)
    key = lax.broadcasted_iota(jnp.int32, (span, rows), 0) - (span - rows)
    past = key <= lax.broadcasted_iota(jnp.int32, (span, rows), 1)
    scores = []
    for q in qs:
        q = q * jnp.asarray(scale, q.dtype)
        zero = jnp.zeros_like(q)
        stacked = jnp.concatenate(
            [
                jnp.concatenate([jnp.where(even, q, zero), picks[0]], axis=1),
                jnp.concatenate([jnp.where(even, zero, q), picks[1]], axis=1),
            ],
            axis=0,
        )
        scores.append(
            lax.dot_general(
                wide, stacked, (((1,), (1,)), ((), ())), preferred_element_type=jnp.float32
            )
        )
    parts = []
    for score, gate, mask in zip(scores, row_gates, masks):
        for n in range(2):
            part = score[:, n * rows : (n + 1) * rows] + gate[n : n + 1]
            parts.append(jnp.where(past, part, -jnp.inf) if mask else part)
    tops = [jnp.max(part, axis=0, keepdims=True) for part in parts]
    exps = [jnp.exp(part - top) for part, top in zip(parts, tops)]
    totals = [jnp.sum(e, axis=0, keepdims=True) for e in exps]
    results = []
    for i in range(len(qs)):
        probs = jnp.concatenate([exps[2 * i], exps[2 * i + 1]], axis=1).astype(v.dtype)
        sums = lax.dot_general(
            v, probs, (((0,), (0,)), ((), ())), preferred_element_type=jnp.float32
        )
        first = sums[:head_size, :rows] * (1.0 / totals[2 * i])
        second = sums[head_size:, rows:] * (1.0 / totals[2 * i + 1])
        lse = [tops[2 * i + n] + jnp.log(totals[2 * i + n]) for n in range(2)]
        results.append((jnp.concatenate([first, second], axis=0), jnp.concatenate(lse, axis=0)))
    return results


def layer_kernel(
    sizes, q_hbm, k_hbm, v_hbm, g_hbm, w_hbm, out_ref,
    q_own, q_in, kv_own, kv_in, g_in, g_row, g_stage, g_key, o_out, s_out, o_in, s_in, o_own, s_own,
    o_far, s_far, total, heads, w_buf, one_part, two_parts,
    in_rs, o_rs, snd, g_rs, g_ss, w_rs, loc, seen_sem,
):
    sp, chunks, head_size, scale = sizes
    z, d = lax.axis_index("sp"), lax.axis_index("dp")
    rows = q_own.shape[0]
    half = w_buf.shape[1] // 2
    core, xs, ys = flip(d, 1), flip(d, 2), flip(d, 4)

    def cols(c):
        return pl.ds(pl.multiple_of(c * LANES, LANES), LANES)

    def remote(src, dst, ss, rs, **device):
        return pltpu.make_async_remote_copy(
            src_ref=src, dst_ref=dst, send_sem=ss, recv_sem=rs,
            device_id=device, device_id_type=MESH,
        )

    def arrived(ref, sem):
        remote(ref, ref, snd.at[0], sem, dp=core).wait_recv()

    def sent(ref, sem):
        remote(ref, ref, sem, w_rs.at[0], dp=core).wait_send()

    local = [
        pltpu.make_async_copy(w_hbm, w_buf.at[0], loc.at[0]),
        pltpu.make_async_copy(q_hbm.at[0], q_own, loc.at[1]),
        pltpu.make_async_copy(g_hbm.at[0], g_in.at[z], loc.at[2]),
        pltpu.make_async_copy(k_hbm.at[0], kv_own.at[0], loc.at[3]),
        pltpu.make_async_copy(v_hbm.at[0], kv_own.at[1], loc.at[3]),
    ]
    for copy in local:
        copy.start()

    barrier = pltpu.get_barrier_semaphore()
    @pl.when(z > 0)
    def _():
        pl.semaphore_signal(barrier, inc=1, device_id={"sp": z - 1}, device_id_type=MESH)

    @pl.when(z < sp - 1)
    def _():
        pl.semaphore_signal(barrier, inc=1, device_id={"sp": z + 1}, device_id_type=MESH)

    for peer in (core, xs, ys):
        pl.semaphore_signal(barrier, inc=1, device_id={"dp": peer}, device_id_type=MESH)
    g_stage[...] = jnp.zeros_like(g_stage)
    pl.semaphore_wait(
        barrier, 3 + (z > 0).astype(jnp.int32) + (z < sp - 1).astype(jnp.int32)
    )

    for teller, pair in ((HUB + 1, (HUB, HUB + 2)), (HUB, (HUB - 1, HUB + 1))):
        @pl.when(z == teller)
        def _():
            for target in pair:
                pl.semaphore_signal(
                    seen_sem, inc=1, device_id={"sp": target},
                    device_id_type=MESH,
                )

    def gate_copy(owner, target, relayed=0):
        late = owner == HUB + 2 and target == HUB
        return remote(
            g_in.at[owner], g_in.at[owner], g_ss.at[relayed], g_rs.at[1 if late else 0], sp=target
        )

    def q_copy(c, slot, target):
        lone = slot == 1 and target == HUB and c == 0
        return remote(
            q_own.at[:, cols(c)], q_in.at[slot, :, cols(c)], snd.at[0],
            in_rs.at[chunks if lone else c], sp=target,
        )

    def kv_copy(c):
        return remote(
            kv_own.at[:, :, cols(c)], kv_in.at[:, :, cols(c)], snd.at[0], in_rs.at[c], sp=HUB
        )

    depth = w_buf.shape[1]
    shed = depth // 8
    odd = z % 2
    parts = {}
    for slot, front, back in ((2, 0, half), (4, half, 0)):
        parts[slot, "first"] = (front, half // 2)
        parts[slot, "second"] = (front + half // 2, half // 2)
        parts[slot, "lent"] = (back + 2 * shed * (1 - odd), 2 * shed)
        parts[slot, "rest"] = (back + shed * (1 + odd), shed)
        parts[slot, "given"] = (back + 3 * shed * odd, shed)
        parts[slot, "swap"] = (back + 3 * shed * (1 - odd), shed)
        parts[slot, "wide"] = (back, 2 * shed)
        parts[slot, "some"] = (back + 5 * shed // 2, 3 * shed // 2)
        parts[slot, "bit"] = (back + 2 * shed, shed // 2)
        thin = THIN * shed // 4
        parts[slot, "thin"] = (back + 4 * shed - thin, thin)
        parts[slot, "most"] = (back + 2 * shed, 2 * shed - thin)
    alias = {"wide": "given", "some": "given", "bit": "rest", "thin": "given", "most": "rest"}
    names = ["first", "second", "rest", "lent", "given"]

    for slot in (2, 4):
        start, size = parts[slot, "second"]
        parts[slot, "kept"] = (start, size // 2)
        parts[slot, "moved"] = (start + size // 2, size // 2)
    lasts = ["first", "kept", "moved"]

    def w_sem(slot, name):
        if name is None:
            return w_rs.at[slot // 3]
        if slot in (2, 4):
            return w_rs.at[3 + names.index(name)]
        if slot == 6:
            return w_rs.at[8 + lasts.index(name)]
        return w_rs.at[11 + (slot != 7)]

    def w_both(slot, name, size):
        arrived(w_buf.at[0, pl.ds(0, 2 * size)], w_sem(slot, name))

    def w_ref(slot, rows_of):
        start, size = rows_of
        return w_buf.at[slot, pl.ds(pl.multiple_of(start, 16), size)]

    def w_copy(slot, into, rows_of, ss, rs, **device):
        remote(w_ref(slot, rows_of), w_ref(into, rows_of), snd.at[ss], rs, **device).start()

    def w_first():
        def spread(name):
            w_copy(0, 2, parts[2, name], 4, w_sem(2, alias.get(name, name)), dp=xs)
            w_copy(0, 4, parts[4, name], 4, w_sem(4, alias.get(name, name)), dp=ys)

        spread("lent")
        w_copy(0, 1, (0, depth), 1, w_sem(1, None), dp=core)
        spread("first")
        spread("second")

        @pl.when(z == HUB + 1)
        def _():
            spread("rest")

        @pl.when(z == HUB + 2)
        def _():
            spread("most")

        @pl.when(z == HUB)
        def _():
            spread("bit")

    turns = {2: (4, ys), 4: (2, xs)}

    def w_got(name):
        w_both(2, alias.get(name, name), parts[2, name][1])
        for slot in (2, 4):
            piece = parts[slot, name]
            peer = turns[slot][1]
            if name == "first":
                w_copy(slot, 6, piece, 4, w_sem(6, "first"), dp=peer)
            if name == "second":
                w_copy(slot, 6, parts[slot, "kept"], 4, w_sem(6, "kept"), dp=peer)

                @pl.when(d % 2 == 1)
                def _():
                    w_copy(slot, 6, parts[slot, "moved"], 4, w_sem(6, "moved"), dp=peer)

            into = w_sem(slot + 1, "second" if name == "second" else None)
            w_copy(slot, slot + 1, piece, 1, into, dp=core)

    def w_cross():
        @pl.when(d % 2 == 1)
        def _():
            w_both(3, "second", half // 2)
            for slot in (2, 4):
                w_copy(slot + 1, 7, parts[slot, "moved"], 4, w_sem(7, "moved"), dp=turns[slot][1])

    def w_lend():
        for giver, sends in (
            (0, [(2, "some", 1)]),
            (1, [(2, "lent", 0), (4, "lent", 0)]),
            (2, [(2, "thin", 3), (4, "thin", 3), (4, "some", 1)]),
            (3, [(2, "swap", 2), (4, "swap", 2)]),
        ):
            @pl.when(z == giver)
            def _():
                for slot, name, target in sends:
                    w_copy(slot, slot, parts[slot, name], 5, w_sem(slot, "given"), sp=target)

    def w_diag(name):
        part = "kept" if name == "second" else name
        w_both(6, part, parts[2, part][1])
        for slot in (2, 4):
            w_copy(6, 7, parts[slot, part], 1, w_sem(7, None), dp=core)
        if name == "second":
            @pl.when(d % 2 == 1)
            def _():
                w_both(6, "moved", shed)
                for slot in (2, 4):
                    w_copy(6, 7, parts[slot, "moved"], 1, w_sem(7, None), dp=core)
                w_both(7, "moved", shed)
                for slot in (2, 4):
                    w_copy(7, 6, parts[slot, "moved"], 1, w_sem(6, "moved"), dp=core)

    def w_odd():
        arrived(w_buf.at[pl.ds(0, 2), pl.ds(0, depth - 2 * shed)], w_sem(3, None))

        @pl.when(d % 2 == 0)
        def _():
            w_both(3, "second", half // 2)

    def w_last():
        @pl.when(d % 2 == 0)
        def _():
            arrived(w_buf.at[7], w_sem(7, None))
            w_both(6, "moved", shed)

        @pl.when(d % 2 == 1)
        def _():
            arrived(w_buf.at[7, pl.ds(0, depth - 2 * shed)], w_sem(7, None))

    local[0].wait()
    w_first()
    for copy in local[1:3]:
        copy.wait()
    pltpu.make_async_copy(kv_own, kv_own, loc.at[3]).wait()

    for owner, target in ((0, 1), (1, 0), (1, 2), (2, 1), (2, 3), (3, 2)):
        @pl.when(z == owner)
        def _():
            gate_copy(owner, target).start()

    def kv_start(start, stop):
        for c in range(start, stop):
            kv_copy(c).start()

    def q_start(start, stop, slot, target):
        for c in range(start, stop):
            q_copy(c, slot, target).start()

    @pl.when(z == 0)
    def _():
        kv_start(0, 1)
        pl.semaphore_wait(seen_sem, 1)
        gate_copy(0, 2).start()
        kv_start(1, chunks)

    @pl.when(z == HUB + 1)
    def _():
        q_start(0, 1, 0, HUB)
        pl.semaphore_wait(seen_sem, 1)
        gate_copy(2, 0).start()
        q_start(1, chunks, 0, HUB)

    @pl.when(z == HUB + 2)
    def _():
        q_start(0, 1, 1, HUB + 1)
        pl.semaphore_wait(seen_sem, 1)
        gate_copy(3, 1).start()
        q_start(0, 1, 1, HUB)
        q_start(1, 2, 1, HUB)
        for c in range(1, chunks):
            q_start(c, c + 1, 1, HUB + 1)
            if c + 1 < chunks:
                q_start(c + 1, c + 2, 1, HUB)

    @pl.when(z == HUB)
    def _():
        pl.semaphore_wait(seen_sem, 1)
        gate_copy(1, 3).start()

    @pl.when(z != HUB)
    def _():
        w_got("lent")
        w_lend()

    @pl.when(z == 0)
    def _():
        w_got("first")

    @pl.when(z == HUB)
    def _():
        arrived(g_in.at[pl.ds(0, sp - 2)], g_rs.at[0])

    @pl.when(z != HUB)
    def _():
        arrived(g_in.at[pl.ds(0, sp - 1)], g_rs.at[0])

    per = g_in.shape[1]

    def row_gates(owners):
        for owner in owners:
            for at in range(per):
                c, n = divmod(owner * per + at, 2)
                g_row[c, n : n + 1, :] = g_in[owner, at : at + 1, :]

    def key_gates(block, owners):
        for owner in owners:
            rest = -g_in[owner, :, pl.ds(pl.multiple_of(block * rows, LANES), rows)]
            for n in range(3):
                piece = rest.astype(jnp.bfloat16).astype(jnp.float32)
                rest = rest - piece
                at = n * SPLIT + owner * per
                g_stage[at : at + per, :] = piece
        return g_stage[...].T.astype(g_key.dtype)

    def hub_gates(owners):
        row_gates(owners)
        for n in range(2):
            g_key[n] = key_gates(n + HUB - 1, range(owners[-1] + 1))

    @pl.when(z == HUB)
    def _():
        hub_gates(range(HUB + 2))

    @pl.when(z != HUB)
    def _():
        row_gates(range(sp))
        g_key[1] = key_gates(z, range(sp))

    def work(c, qs, blocks, both, masks):
        k = kv_own[0, :, cols(c)]
        v = kv_own[1, :, cols(c)]
        gates = g_key[1]
        if both:
            k = jnp.concatenate([kv_in[0, :, cols(c)], k], axis=0)
            v = jnp.concatenate([kv_in[1, :, cols(c)], v], axis=0)
            gates = jnp.concatenate([g_key[0], gates], axis=0)
        rows_of = [
            g_row[c, :, pl.ds(pl.multiple_of(block * rows, LANES), rows)] for block in blocks
        ]
        return attend(
            c, [q[:, cols(c)] for q in qs], rows_of, k, v, gates, masks, scale, head_size
        )

    def finish(c, result):
        heads[:, cols(c)] = result.astype(heads.dtype).T

    def put(c, slot, result, lse):
        o_out[slot, c] = result.astype(o_out.dtype)
        s_out[slot, c] = lse

    def give(c, slot, into, target):
        remote(s_out.at[slot, c], s_in.at[into, c], snd.at[3], o_rs.at[c], sp=target).start()
        remote(o_out.at[slot, c], o_in.at[into, c], snd.at[2], o_rs.at[c], sp=target).start()

    def merge(*pieces):
        top = functools.reduce(jnp.maximum, [lse for _, lse in pieces])
        scales = [jnp.exp(lse - top) for _, lse in pieces]
        total = 1.0 / functools.reduce(jnp.add, scales)
        scales = [scale * total for scale in scales]
        blocks = []
        for n in range(2):
            span = slice(n * head_size, (n + 1) * head_size)
            terms = [
                result[span].astype(jnp.float32) * scale[n : n + 1]
                for (result, _), scale in zip(pieces, scales)
            ]
            blocks.append(functools.reduce(jnp.add, terms))
        return jnp.concatenate(blocks, axis=0), top - jnp.log(total)

    def on(c, step, run, *args):
        @pl.when(c == step)
        def _():
            run(*args)

    cut = chunks // 2
    width = w_buf.shape[2]

    def joined(c):
        return JOINED[0] <= c < JOINED[1]

    def runs(start, stop):
        at = start
        while at < stop:
            end = at + 1
            while end < stop and joined(end) == joined(at):
                end += 1
            yield at, end, joined(at)
            at = end


    def product(slot, start, stop):
        span = pl.ds(start * LANES, (stop - start) * LANES)
        return jnp.dot(heads[:, span], w_buf[slot, span], preferred_element_type=jnp.float32)

    def store(slot, block):
        owner = d
        for bit in (1, 2, 4):
            if slot & bit:
                owner = flip(owner, bit)
        out_ref[0, :, pl.ds(pl.multiple_of(owner * width, LANES), width)] = block.astype(
            out_ref.dtype
        )

    def project(slot):
        store(slot, product(slot, 0, chunks))

    def remain(start):
        for n, slot in enumerate(EARLY):
            store(slot, total[n] + product(slot, start, chunks))

    def gather(stop):
        arrived(w_buf.at[1], w_sem(1, None))
        for n, slot in enumerate(EARLY):
            if stop == chunks:
                project(slot)
            else:
                total[n] = product(slot, 0, stop)

    def ends(stop):
        @pl.when(d % 2 == 0)
        def _():
            w_diag("second")

        gather(stop)

        @pl.when(d % 2 == 1)
        def _():
            w_diag("second")

    @pl.when(z == 0)
    def _():
        @pl.loop(0, chunks // 2)
        def _(pair):
            for n in range(2):
                c = 2 * pair + n
                finish(c, work(c, [q_own], [z], False, [True])[0][0])

        w_got("second")
        w_got("wide")
        w_cross()
        gather(chunks)
        w_diag("first")
        w_diag("second")

    @pl.when(z == HUB)
    def _():
        def far_give(c, joint):
            if joint:
                give(c, 1, 1, HUB + 1)
            else:
                give(c, 1, 0, HUB + 2)

        def hub(c, joint):
            arrived(w_buf.at[0, pl.ds(0, 2 * rows)], in_rs.at[c])
            far, near, own = work(
                c, [q_in.at[1], q_in.at[0], q_own], [HUB + 2, HUB + 1, HUB], True, [False, False, True]
            )
            put(c, 1, *far)
            put(c, 0, *near)
            far_give(c, joint)
            give(c, 0, 0, HUB + 1)
            finish(c, own[0])

        arrived(w_buf.at[0, pl.ds(0, 3 * rows // 2)], in_rs.at[0])
        near, own = work(0, [q_in.at[0], q_own], [HUB + 1, HUB], True, [False, True])
        put(0, 0, *near)
        give(0, 0, 0, HUB + 1)
        finish(0, own[0])
        arrived(g_in.at[0], g_rs.at[1])
        gate_copy(0, 3, 1).start()
        gate_copy(3, 0, 1).start()
        hub_gates(range(HUB + 2, sp))
        arrived(w_buf.at[0, pl.ds(0, rows // 2)], in_rs.at[chunks])
        put(0, 1, *work(0, [q_in.at[1]], [HUB + 2], True, [False])[0])
        far_give(0, joined(0))
        w_got("lent")
        w_lend()

        for start, stop, joint in runs(1, chunks):
            @pl.loop(start, stop)
            def _(c):
                on(c, 2 + d % 2, w_got, "first")
                on(c, 4 + d % 2, w_got, "second")

                @pl.when(c == chunks - 1)
                def _():
                    w_got("bit")
                    w_cross()

                    @pl.when(d % 2 == 1)
                    def _():
                        w_diag("first")

                hub(c, joint)

        @pl.when(d % 2 == 0)
        def _():
            w_diag("first")

        w_got("some")
        ends(chunks)

    @pl.when(z == HUB + 1)
    def _():
        def near(c, joint):
            arrived(q_in.at[1, :, cols(c)], in_rs.at[c])
            far, own = work(c, [q_in.at[1], q_own], [HUB + 2, HUB + 1], False, [False, True])
            if joint:
                o_far[c], s_far[c] = far
            else:
                put(c, 1, *far)
                give(c, 1, 1, HUB + 2)
            o_own[c], s_own[c] = own

        def join(c):
            arrived(two_parts if joined(c) else one_part, o_rs.at[c])
            if joined(c):
                put(c, 1, *merge((o_far[c], s_far[c]), (o_in[1, c], s_in[1, c])))
                give(c, 1, 1, HUB + 2)
            finish(c, merge((o_own[c], s_own[c]), (o_in[0, c], s_in[0, c]))[0])

        for start, stop, joint in runs(0, cut):
            @pl.loop(start, stop)
            def _(c):
                on(c, 3, w_got, "first")
                near(c, joint)

        for c in range(cut, chunks):
            join(c - cut)
            if c == cut + 1:
                w_got("second")
            if c == chunks - 1:
                join(cut)
                w_got("rest")
                w_cross()
            near(c, joined(c))
        w_diag("first")
        w_got("given")
        for c in range(chunks - 3, chunks - 2):
            join(c)

        @pl.when(d % 2 == 0)
        def _():
            w_diag("second")

        join(chunks - 2)
        gather(chunks - 1)

        @pl.when(d % 2 == 1)
        def _():
            w_diag("second")

        join(chunks - 1)
        w_odd()

        @pl.when(d % 2 == 0)
        def _():
            w_last()
            remain(chunks - 1)
            for slot in (3, 5, 6, 7):
                project(slot)

        @pl.when(d % 2 == 1)
        def _():
            remain(chunks - 1)
            for slot in (3, 5):
                project(slot)
            w_last()
            for slot in (6, 7):
                project(slot)

    @pl.when(z == HUB + 2)
    def _():
        @pl.loop(0, chunks // 2)
        def _(pair):
            for n in range(2):
                c = 2 * pair + n
                o_own[c], s_own[c] = work(c, [q_own], [z], False, [True])[0]

        def join(c):
            arrived(one_part if joined(c) else two_parts, o_rs.at[c])
            pieces = [(o_own[c], s_own[c]), (o_in[1, c], s_in[1, c])]
            if not joined(c):
                pieces.append((o_in[0, c], s_in[0, c]))
            finish(c, merge(*pieces)[0])

        w_got("first")
        w_got("second")
        w_got("most")
        w_cross()
        w_diag("first")
        w_got("thin")
        for c in range(cut - 1):
            join(c)

        @pl.when(d % 2 == 0)
        def _():
            w_diag("second")

        join(cut - 1)
        gather(cut)

        @pl.when(d % 2 == 1)
        def _():
            w_diag("second")

        for c in range(cut, chunks):
            join(c)
        w_odd()
        w_last()
        remain(cut)
        for slot in (3, 5, 6, 7):
            project(slot)

    @pl.when(z <= HUB)
    def _():
        w_odd()
        for slot in (3, 5):
            project(slot)
        w_last()
        for slot in (6, 7):
            project(slot)

    for parity in range(2):
        @pl.when(d % 2 == parity)
        def _():
            moved = (2 * parity - 1) * shed
            sent(w_buf.at[:, pl.ds(0, depth // 2 + moved // 4)], snd.at[1])
            for plane in range(sp):
                @pl.when(z == plane)
                def _():
                    each = 5 * depth // 8 + (0, shed // 4, shed // 2, shed - THIN * shed // 8)[plane] + moved // 2
                    sent(w_buf.at[pl.ds(0, 4), pl.ds(0, each)], snd.at[4])

    for giver, count in enumerate((6, 16, 6 + 2 * THIN, 8)):
        @pl.when(z == giver)
        def _():
            sent(w_buf.at[0, pl.ds(0, count * shed // 4)], snd.at[5])

    @pl.when((z == 0) | (z == HUB + 2))
    def _():
        sent(g_in.at[pl.ds(0, 2)], g_ss.at[0])
        sent(kv_own, snd.at[0])

    @pl.when((z == HUB) | (z == HUB + 1))
    def _():
        sent(g_in.at[pl.ds(0, 3)], g_ss.at[0])

    @pl.when(z == HUB)
    def _():
        sent(g_in.at[pl.ds(0, 2)], g_ss.at[1])
        sent(o_out, snd.at[2])
        sent(s_out, snd.at[3])

    @pl.when(z == HUB + 1)
    def _():
        sent(q_own, snd.at[0])
        sent(o_out.at[1], snd.at[2])
        sent(s_out.at[1], snd.at[3])


def fused_shards(sp, queries, keys, values, cum_gates, out_weight):
    _, rows, width = queries.shape
    _, per, length = cum_gates.shape
    head_size = width // (per * sp)
    depth, block = out_weight.shape
    dp = 8
    chunks = width // LANES
    bf16, f32 = queries.dtype, jnp.float32
    dma = pltpu.SemaphoreType.DMA
    return pl.pallas_call(
        functools.partial(layer_kernel, (sp, chunks, head_size, head_size ** (-0.5))),
        out_shape=jax.ShapeDtypeStruct((1, rows, block * dp), bf16),
        in_specs=[pl.BlockSpec(memory_space=pltpu.HBM)] * 5,
        out_specs=pl.BlockSpec(memory_space=pltpu.VMEM),
        scratch_shapes=[
            pltpu.VMEM((rows, width), bf16),
            pltpu.VMEM((2, rows, width), bf16),
            pltpu.VMEM((2, rows, width), bf16),
            pltpu.VMEM((2, rows, width), bf16),
            pltpu.VMEM((sp, per, length), f32),
            pltpu.VMEM((chunks, 2, length), f32),
            pltpu.VMEM((LANES, rows), f32),
            pltpu.VMEM((2, rows, LANES), bf16),
            pltpu.VMEM((2, chunks, LANES, rows), bf16),
            pltpu.VMEM((2, chunks, 2, rows), f32),
            pltpu.VMEM((2, chunks, LANES, rows), bf16),
            pltpu.VMEM((2, chunks, 2, rows), f32),
            pltpu.VMEM((chunks, LANES, rows), f32),
            pltpu.VMEM((chunks, 2, rows), f32),
            pltpu.VMEM((chunks, LANES, rows), f32),
            pltpu.VMEM((chunks, 2, rows), f32),
            pltpu.VMEM((len(EARLY), rows, block), f32),
            pltpu.VMEM((rows, width), bf16),
            pltpu.VMEM((dp, depth, block), bf16),
            pltpu.VMEM((LANES // 4 + 1, 2, rows), f32),
            pltpu.VMEM((LANES // 2 + 2, 2, rows), f32),
            dma((chunks + 1,)), dma((chunks,)), dma((6,)), dma((2,)), dma((2,)), dma((13,)), dma((4,)),
            pltpu.SemaphoreType.REGULAR,
        ],
        compiler_params=pltpu.CompilerParams(collective_id=0, has_side_effects=True, vmem_limit_bytes=16 * 2**20),
        name="layer",
    )(*(pltpu.with_memory_space_constraint(x, pltpu.HBM) for x in (queries, keys, values, cum_gates, out_weight)))


def route(sp, dp, queries, keys, values, cum_gates, out_weight):
    _, rows, width = queries.shape
    head_size = width // (cum_gates.shape[1] * sp)
    fits = (
        sp == HUB + 3
        and dp == 8
        and rows == LANES
        and 2 * head_size == LANES
        and width == 8 * LANES
        and out_weight.shape[0] % (2 * LANES) == 0
        and cum_gates.shape[1] * sp <= SPLIT
        and out_weight.shape[1] % (2 * LANES) == 0
    )
    if fits:
        return fused_shards(sp, queries, keys, values, cum_gates, out_weight)
    return shards(queries, keys, values, cum_gates, out_weight)


def solution(mesh):
    in_specs = (
        P("dp", "sp", None),
        P("dp", "sp", None),
        P("dp", "sp", None),
        P("dp", "sp", None),
        P(None, "dp"),
    )
    out_specs = P("dp", "sp", None)
    body = functools.partial(route, mesh.shape["sp"], mesh.shape["dp"])
    return jax.shard_map(body, mesh=mesh, in_specs=in_specs, out_specs=out_specs, check_vma=False)
```
